128 devices in a mesh: sp: 64 (over z, y, x), tp: 2 (over core).
Axes of the slice: x: 4, y: 4, z: 4, core: 2. Of those that a mesh axis runs over, the one named last changes fastest.
Arguments:
- resid: bfloat16 [16384, 2048], P(('sp', 'tp')), may hold values from -3 to 3
- queries: bfloat16 [16384, 1024], P('sp', 'tp'), may hold values from -8 to 8
- keys: bfloat16 [16384, 256], P('sp', 'tp'), may hold values from -8 to 8
- values: bfloat16 [16384, 256], P('sp', 'tp'), may hold values from -6 to 6
- docs: int32 [16384], P('sp'), may hold values from 0 to 15, never falling along the last dimension, each value on 1 to 8192 neighbouring positions
- sink: float32 [8], P('tp'), may hold values from 2 to 6
- w_out: bfloat16 [1024, 2048], replicated, may hold values from -0.375 to 0.375
- norm_gain: float32 [2048], replicated, may hold values from 0.1 to 1.9
- w_gate: bfloat16 [64, 2048, 1024], P('sp', None, 'tp'), may hold values from -0.125 to 0.125
- w_up: bfloat16 [64, 2048, 1024], P('sp', None, 'tp'), may hold values from -0.125 to 0.125
- w_down: bfloat16 [64, 1024, 2048], P('sp', 'tp'), may hold values from -0.1875 to 0.1875
- expert_ids: int32 [16384, 2], P(('sp', 'tp')), may hold values from 0 to 63, all different within a row; in each aligned block of 128 rows (0 to 127, 128 to 255, ...) at most 8 rows name the same one
- route_weights: float32 [16384, 2], P(('sp', 'tp')), may hold values from 0.1 to 0.9
Outputs:
- layer_out: bfloat16 [16384, 2048], P(('sp', 'tp'))
The draws below stay inside these ranges and needn't reach their ends.
Inputs may be any that keep to these rules, and one draw needn't show every extreme that they name: `docs`: document numbers never fall along the sequence; a document holds at most 8192 positions. `expert_ids`: each row names 2 different experts. The rows of one device (aligned blocks of 256 // 2 rows) name one expert at most 8 times, and in every draw some expert is named exactly 8 times by some device.
All inputs are finite; a program needn't handle non-finite values.
Results may differ from the reference program's by a relative error of at most 0.007.
Values may be sent and summed in bfloat16 or wider, within the bound.
A program may use at most 128 MiB of HBM per device.

```python
import math
import jax
import jax.numpy as jnp
import numpy as np
from jax import lax

D = 2048
QUERY_HEADS = 8
KEY_VALUE_HEADS = 2
HEAD_WIDTH = 128
WINDOW_RADIUS = 128
FF = 1024
TOP_K = 2
TOK_DEV = 256
SEQUENCE_TOKENS = 16384
EXPERTS = 64
CAP = 8
DOCS = 16
LONGEST = 8192
N_SP = 64
N_TP = 2


def query_key_pair(key):
    base = jax.random.fold_in(key, 7)
    kq, key_window = jax.random.split(base)
    keys = jnp.clip(jax.random.normal(key_window, (SEQUENCE_TOKENS, KEY_VALUE_HEADS * HEAD_WIDTH), jnp.float32), -6.0, 6.0)
    queries = jnp.clip(1.5 * jax.random.normal(kq, (SEQUENCE_TOKENS, QUERY_HEADS * HEAD_WIDTH), jnp.float32), -8.0, 8.0)
    return (queries, keys)


def draw_queries(key, part):
    return query_key_pair(key)[0].astype(jnp.bfloat16)


def draw_keys(key, part):
    return query_key_pair(key)[1].astype(jnp.bfloat16)


def levels(own_key, extent, cuts, low, largest):
    gain, own = 1.0, jax.random.fold_in(own_key, 6)
    for position, shards_of in cuts:
        steps = jnp.exp(jax.random.uniform(jax.random.fold_in(own, position), (shards_of,), jnp.float32, low / len(cuts), largest / len(cuts)))
        gain = gain * jnp.repeat(steps, extent[position] // shards_of).reshape([-1 if axis == position else 1 for axis in range(len(extent))])
    return gain


def split_up(count, total, bound, lean):
    weights = [(1 << 20) // math.isqrt(standing ** lean) + 1 for standing in range(2, count + 1)]
    spare, given = total - bound - (count - 1), [1] * (count - 1)
    while spare > 0:
        candidates = [i for i in range(count - 1) if given[i] < bound]
        pool, budget = sum([weights[i] for i in candidates]), spare
        for i in candidates:
            addition = min(bound - given[i], max(1, budget * weights[i] // pool), spare)
            given[i] = given[i] + addition
            spare = spare - addition
    return np.array([bound] + given)


def uneven(own_key, amount, total, reach, slope):
    if amount == 2:
        one = jax.random.randint(own_key, (), max(1, total - reach), min(reach, total - 1) + 1)
        return jnp.stack([one, total - one])
    tallies = jnp.asarray(split_up(amount, total, reach, slope), jnp.int32)
    pairs = (amount - 1) // 2
    giver, taker = tallies[1:1 + 2 * pairs:2], tallies[2:2 + 2 * pairs:2]
    margin = jnp.minimum(giver - 1, reach - taker)
    shifted = jax.random.randint(jax.random.fold_in(own_key, 1), (pairs,), 0, 1 << 20) % (margin + 1)
    tallies = tallies.at[1:1 + 2 * pairs:2].set(giver - shifted).at[2:2 + 2 * pairs:2].set(taker + shifted)
    return tallies[jax.random.permutation(jax.random.fold_in(own_key, 2), amount)]


def deal_out(key, own, number, rows, number_of, top, reach, slope):
    order = jax.random.permutation(key, number_of)
    crowded, ordinary = load_shares(number_of, rows * top, reach, slope, True), load_shares(number_of, rows * top, reach, slope, False)
    places = jnp.arange(number_of)

    def named(sizes, rotation):
        used = int((sizes > 0).sum())
        fixed = max(1, used // 4)
        passed = fixed + (places - fixed + rotation * (used - fixed)) % max(1, number_of - fixed)
        return jnp.zeros((number_of,), jnp.int32).at[order[jnp.where(places < fixed, places, passed)]].set(jnp.asarray(sizes, jnp.int32))

    sizes = jnp.where(number % 4 == 0, named(crowded, number // 4), named(ordinary, number - number // 4 - 1))
    mixed = jax.random.permutation(jax.random.fold_in(own, 3), number_of)
    source_of, receiver = mixed[0:number_of // 2 * 2:2], mixed[1:number_of // 2 * 2:2]
    margin = jnp.minimum(sizes[source_of] - 1, reach - sizes[receiver]) // 2
    margin = jnp.where((source_of == order[0]) | (receiver == order[0]) | (sizes[receiver] == 0), 0, jnp.maximum(margin, 0))
    passed = jax.random.randint(jax.random.fold_in(own, 4), (number_of // 2,), 0, 1 << 20) % (margin + 1)
    sizes = sizes.at[source_of].add(-passed).at[receiver].add(passed)
    members = jnp.searchsorted(jnp.cumsum(sizes), jnp.arange(rows * top), side="right").astype(jnp.int32)
    grid = members.reshape(top, rows).T
    grid = grid[jax.random.permutation(jax.random.fold_in(own, 1), rows)]
    rotation = jax.random.randint(jax.random.fold_in(own, 2), (rows, 1), 0, top)
    return jnp.take_along_axis(grid, (jnp.arange(top)[None, :] + rotation) % top, axis=1)


def load_shares(amount, total, most, slope, full):
    portions = [(1 << 20) // math.isqrt(grade ** slope) + 1 for grade in range(1, amount + 1)]
    largest = most if full else min(most, max(-(-total // amount), total * portions[0] // sum(portions)))
    least = 1 if total - largest >= amount - 1 else 0
    given, surplus = [largest] + [least] * (amount - 1), total - largest - least * (amount - 1)
    while surplus > 0:
        candidates = [i for i in range(1, amount) if given[i] < largest] or [i for i in range(1, amount) if given[i] < most]
        whole, budget = sum([portions[i] for i in candidates]), surplus
        for i in candidates:
            more = min(most - given[i], max(1, budget * portions[i] // whole), surplus)
            given[i] = given[i] + more
            surplus = surplus - more
    return np.array(given)


def normal_values(stream_key, dims, width, bound, cuts=(), kind=jnp.bfloat16):
    level = levels(stream_key, dims, cuts, -0.22, 0.18) if cuts else 1.0
    drawn = jax.random.normal(stream_key, dims, jnp.float32) * width * level
    return jnp.minimum(jnp.maximum(drawn, -bound), bound).astype(kind)


def setup_inputs(seed: int = 0) -> dict:
    seeds = jax.random.split(jax.random.key(seed), 14)
    resid = normal_values(seeds[0], (SEQUENCE_TOKENS, D), 0.5, 3.0, ((0, 128),))
    queries = draw_queries(jax.random.fold_in(seeds[13], 71), 0)
    keys = draw_keys(jax.random.fold_in(seeds[13], 71), 0)
    values = normal_values(seeds[3], (SEQUENCE_TOKENS, KEY_VALUE_HEADS * HEAD_WIDTH), 1.0, 6.0, ((0, 64), (1, 2)))
    docs = jnp.searchsorted(jnp.cumsum(uneven(seeds[4], DOCS, SEQUENCE_TOKENS, LONGEST, 2)), jnp.arange(SEQUENCE_TOKENS), side="right").astype(jnp.int32)
    sink = jnp.clip(2.0 + 4.0 * jax.random.uniform(seeds[5], (QUERY_HEADS,), jnp.float32) ** levels(seeds[5], (QUERY_HEADS,), ((0, 2),), -0.2, 0.2), 2.0, 6.0)
    w_out = normal_values(seeds[6], (QUERY_HEADS * HEAD_WIDTH, D), (QUERY_HEADS * HEAD_WIDTH // 4) ** -0.5, 0.375)
    norm_gain = jnp.clip(1.0 + 0.18 * jax.random.normal(seeds[7], (D,), jnp.float32), 0.1, 1.9)
    w_gate = normal_values(seeds[8], (EXPERTS, D, FF), D ** -0.5, 0.125, ((0, 64), (2, 2)))
    w_up = normal_values(seeds[9], (EXPERTS, D, FF), D ** -0.5, 0.125, ((0, 64), (2, 2)))
    w_down = normal_values(seeds[10], (EXPERTS, FF, D), FF ** -0.5, 0.1875, ((0, 64), (1, 2)))
    expert_ids_keys = jax.random.split(jax.random.fold_in(seeds[11], 1), SEQUENCE_TOKENS // (TOK_DEV // N_TP))
    expert_ids_turns = jax.random.permutation(jax.random.fold_in(seeds[11], 3), SEQUENCE_TOKENS // (TOK_DEV // N_TP))
    expert_ids = jax.vmap(lambda own, number: deal_out(jax.random.fold_in(seeds[11], 2), own, number, TOK_DEV // N_TP, EXPERTS, TOP_K, CAP, 2))(expert_ids_keys, expert_ids_turns).reshape((SEQUENCE_TOKENS, TOP_K))
    route_weights = jnp.clip(0.1 + 0.79999997 * jax.random.uniform(seeds[12], (SEQUENCE_TOKENS, TOP_K), jnp.float32) ** levels(seeds[12], (SEQUENCE_TOKENS, TOP_K), ((0, 128),), -0.2, 0.2), 0.1, 0.9)
    return dict(resid=resid, queries=queries, keys=keys, values=values, docs=docs, sink=sink, w_out=w_out, norm_gain=norm_gain, w_gate=w_gate, w_up=w_up, w_down=w_down, expert_ids=expert_ids, route_weights=route_weights)


eps = 1e-06

def window_band(table):
    return jnp.concatenate([table[:-2], table[1:-1], table[2:]], axis=1)

def reference(resid, queries, keys, values, docs, sink, w_out, norm_gain, w_gate, w_up, w_down, expert_ids, route_weights):
    query_blocks = SEQUENCE_TOKENS // WINDOW_RADIUS
    head_group = QUERY_HEADS // KEY_VALUE_HEADS
    query_block = queries.astype(jnp.float32).reshape(query_blocks, WINDOW_RADIUS, KEY_VALUE_HEADS, head_group, HEAD_WIDTH)
    padded_keys = jnp.pad(keys.astype(jnp.float32), ((WINDOW_RADIUS, WINDOW_RADIUS), (0, 0))).reshape(query_blocks + 2, WINDOW_RADIUS, KEY_VALUE_HEADS, HEAD_WIDTH)
    padded_values = jnp.pad(values.astype(jnp.float32), ((WINDOW_RADIUS, WINDOW_RADIUS), (0, 0))).reshape(query_blocks + 2, WINDOW_RADIUS, KEY_VALUE_HEADS, HEAD_WIDTH)
    dpad = jnp.pad(docs, (WINDOW_RADIUS, WINDOW_RADIUS), constant_values=-1).reshape(query_blocks + 2, WINDOW_RADIUS)
    kband = window_band(padded_keys)
    value_window = window_band(padded_values)
    dband = window_band(dpad)
    scores = jnp.einsum('nqhgd,nkhd->nhgqk', query_block, kband) * HEAD_WIDTH ** (-0.5)
    qpos = jnp.arange(query_blocks)[:, None] * WINDOW_RADIUS + jnp.arange(WINDOW_RADIUS)[None, :]
    kpos = (jnp.arange(query_blocks)[:, None] - 1) * WINDOW_RADIUS + jnp.arange(3 * WINDOW_RADIUS)[None, :]
    offset = kpos[:, None, :] - qpos[:, :, None]
    qdoc = docs.reshape(query_blocks, WINDOW_RADIUS)
    valid = (jnp.abs(offset) <= WINDOW_RADIUS) & (dband[:, None, :] == qdoc[:, :, None])
    valid = valid[:, None, None]
    sink_logits = sink.astype(jnp.float32).reshape(1, KEY_VALUE_HEADS, head_group, 1, 1)
    top = jnp.maximum(lax.optimization_barrier(jnp.max(jnp.where(valid, scores, -jnp.inf), axis=-1, keepdims=True)), sink_logits)
    expo = jnp.where(valid, jnp.exp(scores - top), 0.0)
    denom = lax.optimization_barrier(jnp.sum(expo, axis=-1, keepdims=True)) + jnp.exp(sink_logits - top)
    probs = lax.optimization_barrier((expo / denom).astype(jnp.bfloat16))
    attended = jnp.einsum('nhgqk,nkhd->nqhgd', probs.astype(jnp.float32), value_window).astype(jnp.bfloat16)
    attended = attended.reshape(SEQUENCE_TOKENS, QUERY_HEADS * HEAD_WIDTH)
    mixed = resid.astype(jnp.float32) + jnp.dot(attended, w_out, preferred_element_type=jnp.float32)
    normed = (mixed * lax.rsqrt(lax.optimization_barrier(jnp.mean(mixed * mixed, axis=-1, keepdims=True)) + eps) * norm_gain.astype(jnp.float32)).astype(jnp.bfloat16)
    visits = SEQUENCE_TOKENS * TOP_K
    most = N_SP * N_TP * CAP
    flat = expert_ids.reshape(visits).astype(jnp.int32)
    order = jnp.argsort(flat, stable=True).astype(jnp.int32)
    sorted_e = flat[order]
    counts = jnp.bincount(flat, length=EXPERTS).astype(jnp.int32)
    starts = (jnp.cumsum(counts) - counts).astype(jnp.int32)
    slot_sorted = sorted_e * most + jnp.arange(visits, dtype=jnp.int32) - starts[sorted_e]
    slot = jnp.zeros((visits,), jnp.int32).at[order].set(slot_sorted.astype(jnp.int32))
    owner = jnp.arange(visits, dtype=jnp.int32) // TOP_K
    table = jnp.zeros((EXPERTS * most, D), jnp.bfloat16).at[slot].set(normed[owner]).reshape(EXPERTS, most, D)

    def run(packed):
        rows, wg, wu, wd = packed
        hidden = (jax.nn.silu(jnp.dot(rows, wg, preferred_element_type=jnp.float32)) * jnp.dot(rows, wu, preferred_element_type=jnp.float32)).astype(jnp.bfloat16)
        part = FF // N_TP
        total = jnp.zeros((most, D), jnp.float32)
        for piece in range(N_TP):
            partial_value = jnp.dot(hidden[:, piece * part:(piece + 1) * part], wd[piece * part:(piece + 1) * part], preferred_element_type=jnp.float32).astype(jnp.bfloat16)
            total = total + partial_value.astype(jnp.float32)
        return total.astype(jnp.bfloat16)
    outs = lax.map(run, (table, w_gate, w_up, w_down)).reshape(EXPERTS * most, D)
    got = outs[slot].astype(jnp.float32).reshape(SEQUENCE_TOKENS, TOP_K, D)
    extra = lax.optimization_barrier(jnp.sum(route_weights.astype(jnp.float32)[:, :, None] * got, axis=1))
    return (mixed + extra).astype(jnp.bfloat16)
```

```python
import jax
import jax.numpy as jnp
from jax import lax
from jax.experimental import pallas as pl
from jax.experimental.pallas import tpu as pltpu
from jax.sharding import PartitionSpec as P

MESH = pl.DeviceIdType.MESH
HD = 128
WIN = 128
EPS = 1e-06
SIDE = 4
CAP = 8
HEADS = 4
LOG2E = 1.4426950408889634
SCALE = HD**-0.5 * LOG2E
GROUPS = 4
F32 = jnp.float32
BF16 = jnp.bfloat16


def hops(offset):
    return sum(min(step, SIDE - step) for step in offset)


ORDER = sorted(
    [(i % SIDE, (i // SIDE) % SIDE, i // (SIDE * SIDE)) for i in range(SIDE**3)],
    key=lambda offset: -hops(offset),
)
N_SP = len(ORDER)
BALL = [offset for offset in ORDER if 0 < hops(offset) <= 3]
CORNERS = [(x, y, z) for x in (1, 3) for y in (1, 3) for z in (1, 3)]
PER = N_SP // GROUPS
ROWS = PER * CAP


def chip_at(me, offset, sign):
    dx, dy, dz = ((sign * step) % SIDE for step in offset)
    x, y, z = lax.rem(me, SIDE), lax.rem(me // SIDE, SIDE), me // (SIDE * SIDE)
    x, y, z = lax.rem(x + dx, SIDE), lax.rem(y + dy, SIDE), lax.rem(z + dz, SIDE)
    return (z * SIDE + y) * SIDE + x


def kernel(
    resid, q, k, v, docs, sink, w_out, gain, wg, wu, wd, ids, rw,
    out,
    qbuf, qsend, kwin, vwin, dwin, sinkv, wo, gainv, wgv, wuv, wdv, idsv, rwv, residv,
    tops, sums, parts, weights, sel, comb_hi, comb_lo, att, mixed, normed, outgoing, landed, hid, result, back,
    lsem, xsend, xrecv, wsend, wrecv, dsend, drecv, csend, crecv, selfsem, ready,
):
    me = lax.axis_index("sp")
    tp = lax.axis_index("tp")
    other = 1 - tp
    own_row = pl.multiple_of(WIN * other, WIN)
    oth_row = pl.multiple_of(WIN * tp, WIN)
    halo_row = pl.multiple_of(2 * WIN * tp, WIN)
    near = (lax.rem(me + 1 + (N_SP - 2) * tp, N_SP), tp)
    far = (lax.rem(me + N_SP - 1 + 2 * tp, N_SP), other)
    mate = (me, other)

    barrier = pltpu.get_barrier_semaphore()

    def hello(device):
        pl.semaphore_signal(barrier, inc=1, device_id=device, device_id_type=MESH)

    def load(i, src, dst):
        copy = pltpu.make_async_copy(src, dst, lsem.at[i])
        copy.start()
        return copy

    outside = ((me == 0) & (tp == 0)) | ((me == N_SP - 1) & (tp == 1))
    inside = jnp.logical_not(outside)
    onward = jnp.logical_not(((me == N_SP - 1) & (tp == 0)) | ((me == 0) & (tp == 1)))

    @pl.when(inside)
    def _():
        hello(far)

    for offset in BALL[:20]:
        hello((chip_at(me, offset, 1), tp))
    hello(mate)
    l_k = load(0, k, kwin.at[tp, pl.ds(own_row, 2 * WIN)])
    l_q = load(3, q.at[pl.ds(pl.multiple_of(WIN * tp, WIN), WIN)], qbuf.at[tp])
    l_v = load(1, v, vwin.at[tp, pl.ds(own_row, 2 * WIN)])
    l_d = load(4, docs, dwin.at[pl.ds(other, 2)])
    l_s = load(5, sink, sinkv.at[tp])
    l_qs = load(2, q.at[pl.ds(pl.multiple_of(WIN * other, WIN), WIN)], qsend)
    for offset in BALL[20:]:
        hello((chip_at(me, offset, 1), tp))
    l_ids = load(6, ids, idsv)
    l_rw = load(7, rw, rwv)
    l_gain = load(9, gain, gainv)
    l_res = load(10, resid, residv)
    l_wo = load(11, w_out, wo)
    l_wg = load(12, wg.at[0], wgv.at[0])
    l_wu = load(13, wu.at[0], wuv.at[0])
    l_wd = load(14, wd.at[0], wdv.at[0])

    row = lax.broadcasted_iota(jnp.int32, (WIN, WIN), 0)
    col = lax.broadcasted_iota(jnp.int32, (WIN, WIN), 1)

    def sink_row(g):
        return jnp.concatenate(
            [jnp.broadcast_to(sinkv[g, :, h : h + 1], (1, WIN)) for h in range(HEADS)], axis=1
        )

    def heads_of(g):
        return jnp.concatenate([qbuf[g, :, h * HD : (h + 1) * HD] for h in range(HEADS)], axis=0)

    def score(g, rows, count, bias):
        raw = lax.dot_general(
            kwin[g, pl.ds(rows, count)], heads_of(g), (((1,), (1,)), ((), ())), preferred_element_type=F32
        )
        return raw * SCALE + jnp.concatenate([bias] * HEADS, axis=1)

    def weigh(g, rows, count, expo):
        turned = jnp.transpose(vwin[g, pl.ds(rows, count)].astype(F32)).astype(BF16)
        return jnp.dot(turned, expo.astype(BF16), preferred_element_type=F32)

    def own_part(g):
        scores = score(g, own_row, 2 * WIN, bias_own)
        top = jnp.maximum(jnp.max(scores, axis=0, keepdims=True), sink_row(g) * LOG2E)
        expo = jnp.exp2(scores - top)
        tops[g] = top
        sums[g] = jnp.sum(expo, axis=0, keepdims=True)
        parts[g] = weigh(g, own_row, 2 * WIN, expo)

    def halo_part(g):
        scores = score(g, halo_row, WIN, bias_halo)
        old = tops[g]
        top = jnp.maximum(old, jnp.max(scores, axis=0, keepdims=True))
        expo = jnp.exp2(scores - top)
        shrink = jnp.exp2(old - top)
        denom = sums[g] * shrink + jnp.sum(expo, axis=0, keepdims=True) + jnp.exp2(sink_row(g) * LOG2E - top)
        gain_row = 1.0 / denom
        mixed_heads = (parts[g] * shrink + weigh(g, halo_row, WIN, expo)) * gain_row
        for h in range(HEADS):
            cols = slice(h * HD, (h + 1) * HD)
            att[:, pl.ds(pl.multiple_of(g * HEADS * HD + h * HD, HD), HD)] = jnp.transpose(mixed_heads[:, cols]).astype(BF16)

    l_k.wait()
    l_q.wait()
    l_v.wait()
    l_d.wait()
    l_s.wait()

    def block_bias(b, ok):
        place = b * WIN + row
        key_doc = jnp.transpose(jnp.broadcast_to(dwin[b], (WIN, WIN)))
        keep = (place >= col) & (place <= col + 2 * WIN) & (key_doc == dwin[1])
        return jnp.where(keep if ok is None else keep & ok, 0.0, -jnp.inf)

    bias_own = jnp.concatenate([block_bias(other, None), block_bias(other + 1, None)], axis=0)
    l_qs.wait()
    pl.semaphore_wait(barrier, len(BALL) + 1 + jnp.where(inside, 1, 0))

    def remote(i, src, dst, device, ssem=xsend, rsem=xrecv):
        return pltpu.make_async_remote_copy(
            src_ref=src, dst_ref=dst, send_sem=ssem.at[i], recv_sem=rsem.at[i],
            device_id=device, device_id_type=MESH,
        )

    def send(*args):
        copy = remote(*args)
        copy.start()
        return copy

    near_src = pl.multiple_of(own_row + WIN * other, WIN)
    far_src = pl.multiple_of(own_row + WIN * tp, WIN)
    near_dst = pl.multiple_of(2 * WIN * tp, WIN)
    far_dst = pl.multiple_of(2 * WIN * other, WIN)
    x_near, x_far, x_mate, heavy = [], [], [], []
    for i, win in enumerate((kwin, vwin)):
        x_far.append(remote(3 * i + 1, win.at[tp, pl.ds(far_src, WIN)], win.at[tp, pl.ds(far_dst, WIN)], far))
        x_near.append(remote(3 * i, win.at[tp, pl.ds(near_src, WIN)], win.at[tp, pl.ds(near_dst, WIN)], near))
    x_near.append(remote(6, dwin.at[pl.ds(near_src // WIN, 1)], dwin.at[pl.ds(2 * tp, 1)], near))

    @pl.when(inside)
    def _():
        x_far[0].start()

    @pl.when(onward)
    def _():
        x_near[0].start()

    @pl.when(inside)
    def _():
        x_far[1].start()

    @pl.when(onward)
    def _():
        x_near[1].start()
        x_near[2].start()

    @pl.when(outside)
    def _():
        kwin[:, pl.ds(halo_row, WIN), :] = jnp.zeros((2, WIN, HD), BF16)
        vwin[:, pl.ds(halo_row, WIN), :] = jnp.zeros((2, WIN, HD), BF16)
        dwin[2 * tp] = jnp.zeros((1, WIN), jnp.int32)

    x_mate.append(send(7, qsend, qbuf.at[tp], mate))
    for i, win in enumerate((kwin, vwin)):
        x_mate.append(send(3 * i + 2, win.at[tp, pl.ds(own_row, 2 * WIN)], win.at[tp, pl.ds(oth_row, 2 * WIN)], mate))
    x_mate.append(send(8, sinkv.at[tp], sinkv.at[tp], mate))
    exchange = x_mate
    for offset in CORNERS:
        pl.semaphore_signal(ready, inc=1, device_id=(chip_at(me, offset, 1), tp), device_id_type=MESH)

    own_part(tp)

    l_ids.wait()
    l_rw.wait()
    slot_id = lax.broadcasted_iota(jnp.int32, (N_SP, WIN), 0)
    step = jnp.zeros((N_SP, WIN), jnp.int32)
    for slot, (x, y, z) in enumerate(ORDER):
        step = jnp.where(slot_id == slot, x + SIDE * y + SIDE * SIDE * z, step)
    expert = (
        ((me // 16 + step // 16) & 3) * 16
        + (((me // 4) % 4 + (step // 4) % 4) & 3) * 4
        + ((me % 4 + step % 4) & 3)
    )
    first = idsv[0:1, :] == expert
    second = idsv[1:2, :] == expert
    visits = jnp.where(first | second, 1.0, 0.0)
    weight = jnp.where(first, rwv[0:1, :], 0.0) + jnp.where(second, rwv[1:2, :], 0.0)
    tokens = visits.shape[1]
    before = jnp.where(
        lax.broadcasted_iota(jnp.int32, (tokens, tokens), 0)
        < lax.broadcasted_iota(jnp.int32, (tokens, tokens), 1),
        1.0,
        0.0,
    )
    rank = jnp.dot(visits.astype(BF16), before.astype(BF16), preferred_element_type=F32)
    code = jnp.where(visits > 0.0, rank, -1.0)
    slot_rank = lax.broadcasted_iota(jnp.int32, (N_SP, CAP, tokens), 1).astype(F32)
    hit = jnp.broadcast_to(code.reshape(N_SP, 1, tokens), (N_SP, CAP, tokens)) == slot_rank
    picked = jnp.where(hit, 1.0, 0.0).reshape(N_SP * CAP, tokens)
    sel[...] = picked.astype(BF16)
    weights[...] = weight

    for copy in x_mate:
        copy.wait_recv()
    own_part(other)

    @pl.when(inside)
    def _():
        for copy in x_near:
            copy.wait_recv()

    for i, (src, dst) in enumerate(((wg, wgv), (wu, wuv), (wd, wdv))):
        heavy.append(send(i, src.at[0], dst.at[1], mate, wsend, wrecv))

    bias_halo = block_bias(2 * tp, row >= jnp.where(outside, WIN, 0))
    halo_part(tp)

    @pl.when(inside)
    def _():
        for copy in x_far:
            copy.wait_recv()

    halo_part(other)

    l_res.wait()
    l_wo.wait()
    l_gain.wait()
    width = mixed.shape[1]
    tile = 512
    total = jnp.zeros((tokens, 1), F32)
    for n in range(width // tile):
        cols = slice(n * tile, (n + 1) * tile)
        m = residv[:, cols].astype(F32) + jnp.dot(att[...], wo[:, cols], preferred_element_type=F32)
        mixed[:, cols] = m
        total = total + jnp.sum(m * m, axis=1, keepdims=True)
    factor = lax.rsqrt(total * (1.0 / width) + EPS)
    for n in range(width // tile):
        cols = slice(n * tile, (n + 1) * tile)
        normed[:, cols] = (mixed[:, cols] * factor * gainv[0:1, cols]).astype(BF16)

    def rows_of(slot, count=1):
        return pl.ds(slot * CAP, count * CAP)

    pl.semaphore_wait(ready, len(CORNERS))

    for c in range(GROUPS):
        for n in range(width // tile):
            cols = slice(n * tile, (n + 1) * tile)
            outgoing[c * ROWS : (c + 1) * ROWS, cols] = jnp.dot(
                sel[c * ROWS : (c + 1) * ROWS, :], normed[:, cols], preferred_element_type=F32
            ).astype(BF16)
        for slot in range(c * PER, min((c + 1) * PER, N_SP - 1)):
            pltpu.make_async_remote_copy(
                src_ref=outgoing.at[rows_of(slot)], dst_ref=landed.at[rows_of(slot)],
                send_sem=dsend.at[c], recv_sem=drecv.at[c],
                device_id=(chip_at(me, ORDER[slot], 1), tp), device_id_type=MESH,
            ).start()
    own = pltpu.make_async_copy(outgoing.at[rows_of(N_SP - 1)], landed.at[rows_of(N_SP - 1)], selfsem.at[0])
    own.start()

    scaled = jnp.where(
        sel[...].astype(F32).reshape(N_SP, CAP, tokens) > 0.0, jnp.broadcast_to(weights[...].reshape(N_SP, 1, tokens), (N_SP, CAP, tokens)), 0.0
    ).reshape(N_SP * CAP, tokens)
    turned = jnp.transpose(scaled)
    upper = turned.astype(BF16)
    comb_hi[...] = upper
    comb_lo[...] = (turned - upper.astype(F32)).astype(BF16)

    for copy in (l_wg, l_wu, l_wd):
        copy.wait()
    for copy in heavy:
        copy.wait_recv()

    def remote_rows(c):
        return rows_of(c * PER, PER - 1 if c == GROUPS - 1 else PER)

    half = hid.shape[1] // 2
    ftile = 256
    for c in range(GROUPS):
        pltpu.make_async_copy(outgoing.at[remote_rows(c)], landed.at[remote_rows(c)], drecv.at[c]).wait()
        if c == GROUPS - 1:
            own.wait()
        base = c * ROWS

        for part in range(2):
            def up(n, carry):
                cols = pl.ds(pl.multiple_of(n * ftile, ftile), ftile)
                x = landed[base : base + ROWS, :]
                g = jnp.dot(x, wgv[part, :, cols], preferred_element_type=F32)
                u = jnp.dot(x, wuv[part, :, cols], preferred_element_type=F32)
                h = g * (1.0 / (1.0 + jnp.exp(-g))) * u
                hid[:, pl.ds(pl.multiple_of(part * half + n * ftile, ftile), ftile)] = h.astype(BF16)
                return carry

            lax.fori_loop(0, half // ftile, up, 0)

        def down(n, carry):
            cols = pl.ds(pl.multiple_of(n * ftile, ftile), ftile)
            y = jnp.dot(hid[:, :half], wdv[0, :, cols], preferred_element_type=F32)
            y = y + jnp.dot(hid[:, half:], wdv[1, :, cols], preferred_element_type=F32)
            result[base : base + ROWS, cols] = y.astype(BF16)
            return carry

        lax.fori_loop(0, width // ftile, down, 0)
        for slot in range(c * PER, min((c + 1) * PER, N_SP - 1)):
            pltpu.make_async_remote_copy(
                src_ref=result.at[rows_of(slot)], dst_ref=back.at[rows_of(slot)],
                send_sem=csend.at[c], recv_sem=crecv.at[c],
                device_id=(chip_at(me, ORDER[slot], -1), tp), device_id_type=MESH,
            ).start()
    own_back = pltpu.make_async_copy(result.at[rows_of(N_SP - 1)], back.at[rows_of(N_SP - 1)], selfsem.at[1])
    own_back.start()

    for c in range(GROUPS):
        pltpu.make_async_copy(result.at[remote_rows(c)], back.at[remote_rows(c)], crecv.at[c]).wait()
        if c == GROUPS - 1:
            own_back.wait()
        part = slice(c * ROWS, (c + 1) * ROWS)
        for n in range(width // tile):
            cols = slice(n * tile, (n + 1) * tile)
            extra = jnp.dot(comb_hi[:, part], back[part, cols], preferred_element_type=F32)
            extra = extra + jnp.dot(comb_lo[:, part], back[part, cols], preferred_element_type=F32)
            if c < GROUPS - 1:
                mixed[:, cols] = mixed[:, cols] + extra
            else:
                out[:, cols] = (mixed[:, cols] + extra).astype(BF16)

    for copy in exchange + heavy:
        copy.wait_send()

    @pl.when(inside)
    def _():
        for copy in x_far:
            copy.wait_send()

    @pl.when(onward)
    def _():
        for copy in x_near:
            copy.wait_send()

    for c in range(GROUPS):
        pltpu.make_async_copy(outgoing.at[remote_rows(c)], landed.at[remote_rows(c)], dsend.at[c]).wait()
        pltpu.make_async_copy(result.at[remote_rows(c)], back.at[remote_rows(c)], csend.at[c]).wait()


def local(resid, queries, keys, values, docs, sink, w_out, norm_gain, w_gate, w_up, w_down, expert_ids, route_weights):
    tokens, width = resid.shape
    ff = w_gate.shape[2]
    slots = N_SP * CAP
    vmem = pltpu.VMEM
    dma = pltpu.SemaphoreType.DMA
    return pl.pallas_call(
        kernel,
        out_shape=pltpu.VMEM((tokens, width), BF16),
        in_specs=[pl.BlockSpec(memory_space=pl.ANY)] * 13,
        out_specs=pl.BlockSpec(memory_space=pltpu.VMEM),
        scratch_shapes=[
            vmem((2, tokens, 512), BF16),
            vmem((tokens, 512), BF16),
            vmem((2, 3 * WIN, HD), BF16),
            vmem((2, 3 * WIN, HD), BF16),
            vmem((3, 1, WIN), jnp.int32),
            vmem((2, 1, 4), F32),
            vmem(w_out.shape, BF16),
            vmem((1, width), F32),
            vmem((2, width, ff), BF16),
            vmem((2, width, ff), BF16),
            vmem((2, ff, width), BF16),
            vmem((2, tokens), jnp.int32),
            vmem((2, tokens), F32),
            vmem((tokens, width), BF16),
            vmem((2, 1, HEADS * WIN), F32),
            vmem((2, 1, HEADS * WIN), F32),
            vmem((2, HD, HEADS * WIN), F32),
            vmem((N_SP, tokens), F32),
            vmem((slots, tokens), BF16),
            vmem((tokens, slots), BF16),
            vmem((tokens, slots), BF16),
            vmem((tokens, 8 * HD), BF16),
            vmem((tokens, width), F32),
            vmem((tokens, width), BF16),
            vmem((slots, width), BF16),
            vmem((slots, width), BF16),
            vmem((ROWS, 2 * ff), BF16),
            vmem((slots, width), BF16),
            vmem((slots, width), BF16),
            dma((15,)),
            dma((9,)),
            dma((9,)),
            dma((3,)),
            dma((3,)),
            dma((GROUPS,)),
            dma((GROUPS,)),
            dma((GROUPS,)),
            dma((GROUPS,)),
            dma((2,)),
            pltpu.SemaphoreType.REGULAR,
        ],
        compiler_params=pltpu.CompilerParams(
            collective_id=0, has_side_effects=True, vmem_limit_bytes=60 * 1024 * 1024
        ),
        name="layer",
    )(
        resid, queries, keys, values, docs.reshape(2, 1, WIN), sink.reshape(1, 4), w_out,
        norm_gain.reshape(1, width), w_gate, w_up, w_down, expert_ids.T, route_weights.T,
    )


def solution(mesh):
    in_specs = (
        P(("sp", "tp"), None),
        P("sp", "tp"),
        P("sp", "tp"),
        P("sp", "tp"),
        P("sp"),
        P("tp"),
        P(),
        P(),
        P("sp", None, "tp"),
        P("sp", None, "tp"),
        P("sp", "tp", None),
        P(("sp", "tp"), None),
        P(("sp", "tp"), None),
    )
    out_specs = P(("sp", "tp"), None)
    return jax.shard_map(local, mesh=mesh, in_specs=in_specs, out_specs=out_specs, check_vma=False)
```
